512 devices in a mesh: sp: 16 (over y, x), tp: 32 (over z, core).
Axes of the slice: x: 4, y: 4, z: 16, core: 2. Of those that a mesh axis runs over, the one named last changes fastest.
Arguments:
- tokens: bfloat16 [3, 8192, 4096], P(None, 'sp', 'tp'), may hold values from -6 to 6
- new_token: bfloat16 [3, 1, 4096], P(None, None, 'tp'), may hold values from -6 to 6
- query_weight: bfloat16 [4096, 4096], P(None, 'tp'), may hold values from -0.09375 to 0.09375
- key_weight: bfloat16 [4096, 4096], P(None, 'tp'), may hold values from -0.09375 to 0.09375
- value_weight: bfloat16 [4096, 4096], P(None, 'tp'), may hold values from -0.09375 to 0.09375
- log_decay: float32 [64], P('tp'), may hold values from -0.034 to 0
Outputs:
- state: bfloat16 [3, 64, 64, 64], P(None, 'tp', 'sp')
- read: bfloat16 [3, 4096], P(None, 'tp')
The draws below stay inside these ranges and needn't reach their ends.
All inputs are finite; a program needn't handle non-finite values.
Results may differ from the reference program's by a relative error of at most 0.012.
Values may be sent and summed in bfloat16 or wider, within the bound.
A program may use at most 64 MiB of HBM per device.

```python
import jax
import jax.numpy as jnp
from jax import lax

D = 4096
HEADS = 64
HD = 64
SEQS = 3
SPAN = 512
LEN = 8192
N_SP = 16


def draw_log_decay(key, part):
    choose_key = jax.random.fold_in(key, 11)
    fast_key = jax.random.fold_in(key, 12)
    slow_key = jax.random.fold_in(key, 13)
    chain_len = max(LEN, 64)
    fast_heads = jax.random.randint(choose_key, (HEADS,), 0, 2) == 1
    slow_rates = -jax.random.uniform(slow_key, (HEADS,), jnp.float32, 0.1, 2.0) / chain_len
    fast_rates = -1.0 / jax.random.uniform(fast_key, (HEADS,), jnp.float32, 30.0, 100.0)
    return jnp.where(fast_heads, fast_rates, slow_rates).astype(jnp.float32)


def shard_levels(own_key, dims, shards, low, top_value):
    def one(axis_at, parts):
        heights = jax.random.uniform(jax.random.fold_in(jax.random.fold_in(own_key, 6), axis_at), (parts,), jnp.float32, low / len(shards), top_value / len(shards))
        return jnp.repeat(jnp.exp(heights), dims[axis_at] // parts).reshape((-1,) + (1,) * (len(dims) - axis_at - 1))

    loudness = one(*shards[0])
    for cut in shards[1:]:
        loudness = loudness * one(*cut)
    return loudness


def bell_draw(rng, shape, spread, bound, pieces=(), kind=jnp.bfloat16):
    drawn = jax.random.normal(rng, shape, jnp.float32) * spread
    if len(pieces) > 0:
        drawn = shard_levels(rng, shape, pieces, -0.22, 0.18) * drawn
    return jnp.clip(drawn, min=-bound, max=bound).astype(kind)


def setup_inputs(seed: int = 0) -> dict:
    streams_of = jax.random.split(jax.random.key(seed), 7)
    return {
        "tokens": bell_draw(streams_of[0], (SEQS, LEN, D), 1.0, 6.0, ((1, 16), (2, 32))),
        "new_token": bell_draw(streams_of[1], (SEQS, 1, D), 1.0, 6.0, ((2, 32),)),
        "query_weight": bell_draw(streams_of[2], (D, HEADS * HD), D ** -0.5, 0.09375, ((1, 32),)),
        "key_weight": bell_draw(streams_of[3], (D, HEADS * HD), D ** -0.5, 0.09375, ((1, 32),)),
        "value_weight": bell_draw(streams_of[4], (D, HEADS * HD), D ** -0.5, 0.09375, ((1, 32),)),
        "log_decay": draw_log_decay(jax.random.fold_in(streams_of[6], 71), 0),
    }


def rotate(values, positions):
    half_dim = values.shape[-1] // 2
    inverse = 10000.0 ** (-jnp.arange(half_dim, dtype=jnp.float32) / half_dim)
    angles = positions.astype(jnp.float32)[:, None, None] * inverse[None, None, :]
    cosine = jnp.cos(angles)
    sine_part = jnp.sin(angles)
    first = values[..., :half_dim]
    second = values[..., half_dim:]
    return jnp.concatenate([first * cosine - second * sine_part, first * sine_part + second * cosine], axis=-1)

def group_norm(output):
    centered = output - lax.optimization_barrier(jnp.mean(output, axis=-1, keepdims=True))
    return centered * lax.rsqrt(lax.optimization_barrier(jnp.mean(centered * centered, axis=-1, keepdims=True)) + 1e-05)

def reference(tokens, new_token, query_weight, key_weight, value_weight, log_decay):
    key_scale = HD ** (-0.5)
    positions = jnp.arange(LEN, dtype=jnp.int32)
    to_end = (SPAN - 1 - positions % SPAN).astype(jnp.float32)
    block_ids = jnp.arange(N_SP, dtype=jnp.float32)
    new_position = jnp.full((1,), LEN, jnp.int32)
    query_heads = query_weight.reshape(D, HEADS, HD).transpose(1, 0, 2)
    key_heads = key_weight.reshape(D, HEADS, HD).transpose(1, 0, 2)
    value_heads = value_weight.reshape(D, HEADS, HD).transpose(1, 0, 2)

    def single_head(inputs):
        w_query, w_key, w_value, logarithm_rate = inputs
        projected = jnp.dot(tokens, w_key, preferred_element_type=jnp.float32)[:, :, None, :]
        key_rows = (rotate(projected, positions) * key_scale).astype(jnp.bfloat16)[:, :, 0, :]
        value_rows = jnp.dot(tokens, w_value, preferred_element_type=jnp.float32).astype(jnp.bfloat16)
        weighted = (key_rows.astype(jnp.float32) * jnp.exp(logarithm_rate * to_end)[None, :, None]).astype(jnp.bfloat16)
        weighted = weighted.astype(jnp.float32).reshape(SEQS, N_SP, SPAN, HD)
        value_blocks = value_rows.astype(jnp.float32).reshape(SEQS, N_SP, SPAN, HD)
        segment_states = jnp.einsum('sbtk,sbtv->sbkv', weighted, value_blocks, precision=lax.Precision.HIGHEST)
        carried_state = jnp.exp(logarithm_rate * SPAN * (N_SP - 1 - block_ids))
        closing_state = jnp.einsum('eyzt,y->ezt', segment_states, carried_state, precision=lax.Precision.HIGHEST)
        new_query = rotate(jnp.dot(new_token, w_query, preferred_element_type=jnp.float32)[:, :, None, :], new_position)
        new_query = new_query.astype(jnp.bfloat16)[:, 0, 0, :]
        fresh_key = rotate(jnp.dot(new_token, w_key, preferred_element_type=jnp.float32)[:, :, None, :], new_position)
        fresh_key = (fresh_key * key_scale).astype(jnp.bfloat16)[:, 0, 0, :]
        new_value = jnp.dot(new_token, w_value, preferred_element_type=jnp.float32).astype(jnp.bfloat16)[:, 0, :]
        query_entries = new_query.astype(jnp.float32)
        unscaled_read = jnp.exp(logarithm_rate) * jnp.einsum('bol,bo->bl', closing_state, query_entries, precision=lax.Precision.HIGHEST)
        unscaled_read = unscaled_read + lax.optimization_barrier(jnp.sum(query_entries * fresh_key.astype(jnp.float32), axis=-1, keepdims=True)) * new_value.astype(jnp.float32)
        return (closing_state.astype(jnp.bfloat16), group_norm(unscaled_read).astype(jnp.bfloat16))
    states, reads = lax.map(single_head, (query_heads, key_heads, value_heads, log_decay))
    return (states.transpose(1, 0, 2, 3), reads.transpose(1, 0, 2).reshape(SEQS, HEADS * HD))
```

```python
import functools

import jax
import jax.numpy as jnp
import numpy as np
from jax import lax
from jax.experimental import pallas as pl
from jax.experimental.pallas import tpu as pltpu
from jax.sharding import PartitionSpec as P

HD = 64
MESH = pl.DeviceIdType.MESH
NZ = 16
CH = 256
NCH = 6
HALF = 3
STEPS = 7 * NCH + HALF
LANES = 128


def kernel(
    groups,
    tok_ref,
    new_ref,
    wq_ref,
    wk_ref,
    wv_ref,
    ld_ref,
    state_ref,
    read_ref,
    blocks,
    news,
    weights,
    acc,
    acc_new,
    cos_t,
    sin_t,
    dec_t,
    out_buf,
    in_buf,
    tok_sem,
    w_sem,
    up_send,
    dn_send,
    pt_send,
    up_recv,
    dn_recv,
    pu_recv,
    pd_recv,
    own_recv,
    nu_send,
    nd_send,
    np_send,
    nu_recv,
    nd_recv,
    npu_recv,
    npd_recv,
    nown_recv,
    x_send,
    x_recv,
):
    sp = lax.axis_index("sp")
    tp = lax.axis_index("tp")
    z = tp // 2
    core = tp % 2
    up = ((z + 1) % NZ) * 2 + core
    dn = ((z + NZ - 1) % NZ) * 2 + core
    partner = z * 2 + (1 - core)
    span = NCH // 3 * CH

    own_copies = []
    for ch in range(NCH):
        half, p = ch // 3, ch % 3
        c = pltpu.make_async_copy(
            tok_ref.at[p, pl.ds(half * CH, CH), :], blocks.at[tp * NCH + ch], tok_sem.at[ch]
        )
        c.start()
        own_copies.append(c)
    w_copies = []
    for i, ref in enumerate((wk_ref, wv_ref, wq_ref)):
        c = pltpu.make_async_copy(ref, weights.at[:, pl.ds(i * LANES, LANES)], w_sem.at[i])
        c.start()
        w_copies.append(c)

    barrier = pltpu.get_barrier_semaphore()
    for peer in (up, dn, partner):
        pl.semaphore_signal(barrier, inc=1, device_id=(sp, peer), device_id_type=MESH)
    for d in range(1, groups):
        pl.semaphore_signal(
            barrier, inc=1, device_id=((sp + d) % groups, tp), device_id_type=MESH
        )

    own_new = jnp.concatenate(
        [new_ref[:, 0, :].astype(jnp.float32), jnp.zeros((13, LANES), jnp.float32)], axis=0
    )
    news[tp] = own_new.astype(jnp.bfloat16)

    pl.semaphore_wait(barrier, 3 + groups - 1)

    def remote(src, send, recv, peer, ref=None):
        ref = blocks if ref is None else ref
        return pltpu.make_async_remote_copy(
            src_ref=ref.at[src],
            dst_ref=ref.at[src],
            send_sem=send,
            recv_sem=recv,
            device_id=(sp, peer),
            device_id_type=MESH,
        )

    remote(tp, nu_send.at[0], nu_recv.at[0], up, news).start()
    remote(tp, nd_send.at[0], nd_recv.at[0], dn, news).start()
    remote(tp, np_send.at[15], nown_recv, partner, news).start()
    for ch in range(NCH):
        own_copies[ch].wait()
    for pos in range(NCH):
        cu, cd = pos, (pos + HALF) % NCH
        remote(tp * NCH + cu, up_send, up_recv.at[pos], up).start()
        remote(tp * NCH + cd, dn_send, dn_recv.at[pos], dn).start()
    for ch in range(NCH):
        remote(tp * NCH + ch, pt_send, own_recv.at[ch], partner).start()

    def source(t, down):
        k, pos = t // NCH, t % NCH
        if down:
            sz = (z + 1 + k) % NZ
            ch = (pos + HALF) % NCH
        else:
            sz = (z + NZ - 1 - k) % NZ
            ch = pos
        return k, sz, ch

    lane = lax.broadcasted_iota(jnp.int32, (1, LANES), 1)
    inverse = jnp.zeros((1, LANES), jnp.float32)
    freq = (10000.0 ** (-np.arange(32, dtype=np.float64) / 32)).astype(np.float32)
    for i in range(32):
        inverse = jnp.where(lane % 32 == i, float(freq[i]), inverse)
    first = (lane % HD) < 32
    low = lane < HD
    ld = jnp.where(low, ld_ref[0], ld_ref[1])
    row = lax.broadcasted_iota(jnp.int32, (span, LANES), 0)
    angle = (row + sp * span).astype(jnp.float32) * inverse
    cos_t[...] = jnp.cos(angle) * 0.125
    sin_t[...] = jnp.where(first, -jnp.sin(angle), jnp.sin(angle)) * 0.125
    dec_t[...] = jnp.exp((span - 1 - row).astype(jnp.float32) * ld)
    carried = jnp.exp(ld * (span * (groups - 1 - sp)).astype(jnp.float32))

    for c in w_copies:
        c.wait()

    def lhs(sz, ch):
        return jnp.concatenate(
            [blocks[(2 * sz) * NCH + ch], blocks[(2 * sz + 1) * NCH + ch]], axis=1
        )

    def rows_of(sz):
        return pl.ds(pl.multiple_of(sz * 256, 256), 256)

    def new_dot(sz):
        x = jnp.concatenate([news[2 * sz], news[2 * sz + 1]], axis=1)
        return jnp.dot(x, weights[rows_of(sz), :], preferred_element_type=jnp.float32)

    def kv_dot(sz, ch):
        return jnp.dot(
            lhs(sz, ch), weights[rows_of(sz), 0:256], preferred_element_type=jnp.float32
        )

    remote(partner, np_send.at[15], nown_recv, partner, news).wait_recv()
    acc_new[...] = new_dot(z)
    for ch in range(NCH):
        remote(partner * NCH + ch, pt_send, own_recv.at[ch], partner).wait_recv()
        acc[pl.ds(ch * CH, CH), :] = kv_dot(z, ch)

    def relay(t):
        k, su, cu = source(t, False)
        _, sd, cd = source(t, True)
        bu = (su * 2 + core) * NCH + cu
        bd = (sd * 2 + core) * NCH + cd

        def small():
            nu = su * 2 + core
            nd = sd * 2 + core
            remote(nu, nu_send.at[k], nu_recv.at[k], up, news).wait_recv()

            @pl.when(k < 7)
            def _():
                remote(nu, nu_send.at[k + 1], nu_recv.at[k + 1], up, news).start()
                remote(nd, nd_send.at[k], nd_recv.at[k], dn, news).wait_recv()

                @pl.when(k < 6)
                def _():
                    remote(nd, nd_send.at[k + 1], nd_recv.at[k + 1], dn, news).start()

                remote(nd, np_send.at[k + 8], npd_recv.at[k], partner, news).start()

            remote(nu, np_send.at[k], npu_recv.at[k], partner, news).start()

        if isinstance(t, int):
            if t % NCH == 0:
                small()
        else:
            pl.when(t % NCH == 0)(small)

        def forward():
            remote(bu, up_send, up_recv.at[t + NCH], up).start()

        def forward_down():
            remote(bd, dn_send, dn_recv.at[t + NCH], dn).start()

        remote(bu, up_send, up_recv.at[t], up).wait_recv()
        if isinstance(t, int):
            if t + NCH < STEPS:
                forward()
        else:
            pl.when(t + NCH < STEPS)(forward)
        remote(bu, pt_send, pu_recv.at[t], partner).start()
        remote(bd, dn_send, dn_recv.at[t], dn).wait_recv()
        if isinstance(t, int):
            if t + NCH < STEPS:
                forward_down()
        else:
            pl.when(t + NCH < STEPS)(forward_down)
        remote(bd, pt_send, pd_recv.at[t], partner).start()

    def compute(t):
        k, su, cu = source(t, False)
        _, sd, cd = source(t, True)
        pc = 1 - core

        def small():
            remote(su * 2 + pc, np_send.at[k], npu_recv.at[k], partner, news).wait_recv()
            acc_new[...] += new_dot(su)

            @pl.when(k < 7)
            def _():
                remote(sd * 2 + pc, np_send.at[k], npd_recv.at[k], partner, news).wait_recv()
                acc_new[...] += new_dot(sd)

        if isinstance(t, int):
            if t % NCH == 0:
                small()
        else:
            pl.when(t % NCH == 0)(small)
        remote((su * 2 + pc) * NCH + cu, pt_send, pu_recv.at[t], partner).wait_recv()
        at = pl.ds(pl.multiple_of(cu * CH, CH), CH)
        acc[at, :] += kv_dot(su, cu)
        remote((sd * 2 + pc) * NCH + cd, pt_send, pd_recv.at[t], partner).wait_recv()
        at = pl.ds(pl.multiple_of(cd * CH, CH), CH)
        acc[at, :] += kv_dot(sd, cd)

    last = STEPS - HALF

    def step(t, carry):
        relay(t)
        pl.when(t >= 1)(lambda: compute(t - 1))
        return carry

    lax.fori_loop(0, last + 1, step, 0)

    def turned(x, cosine, sine):
        swapped = jnp.where(first, pltpu.roll(x, LANES - 32, 1), pltpu.roll(x, 32, 1))
        return x * cosine + swapped * sine

    relay(last + 1)
    compute(last)

    new_angle = (groups * span) * inverse
    new_cos = jnp.cos(new_angle)
    new_sin = jnp.where(first, -jnp.sin(new_angle), jnp.sin(new_angle))
    new_k = (turned(acc_new[0:8, 0:128], new_cos, new_sin) * 0.125).astype(jnp.bfloat16)
    new_v = acc_new[0:8, 128:256].astype(jnp.bfloat16).astype(jnp.float32)
    new_q = turned(acc_new[0:8, 256:384], new_cos, new_sin).astype(jnp.bfloat16)
    new_q = new_q.astype(jnp.float32)
    product = new_q * new_k.astype(jnp.float32)

    def head_sums(x):
        lo = jnp.sum(jnp.where(low, x, 0.0), axis=1, keepdims=True)
        hi = jnp.sum(jnp.where(low, 0.0, x), axis=1, keepdims=True)
        return jnp.where(low, lo, hi)

    own_term = head_sums(product) * new_v
    q_cols = jnp.transpose(jnp.concatenate([new_q] * 16, axis=0))
    one = jnp.exp(ld)

    def finish(p):
        total = None
        for half in range(2):
            at = pl.ds(half * CH, CH)
            rows = acc[pl.ds((half * 3 + p) * CH, CH), :]
            keys = turned(rows[:, 0:128], cos_t[at, :], sin_t[at, :]).astype(jnp.bfloat16)
            keys = (keys.astype(jnp.float32) * dec_t[at, :]).astype(jnp.bfloat16)
            part = lax.dot_general(
                keys,
                rows[:, 128:256].astype(jnp.bfloat16),
                (((0,), (0,)), ((), ())),
                preferred_element_type=jnp.float32,
            )
            total = part if total is None else total + part
        tile = jnp.where(low, total[0:HD, :], total[HD:, :]) * carried
        query = jnp.where(low, q_cols[0:HD, p : p + 1], q_cols[HD:, p : p + 1])
        partial = jnp.sum(tile * query, axis=0, keepdims=True) * one
        out_buf[:, pl.ds(p * 4, 4), :] = tile.reshape(groups, HD // groups, LANES)
        out_buf[:, pl.ds(12 + p, 1), :] = jnp.broadcast_to(partial[None], (groups, 1, LANES))

    out_buf[:, pl.ds(15, 1), :] = jnp.zeros((groups, 1, LANES), jnp.float32)
    finish(0)
    relay(last + 2)
    compute(last + 1)
    finish(1)
    compute(last + 2)
    finish(2)

    for d in range(1, groups):
        peer = (sp + d) % groups
        pltpu.make_async_remote_copy(
            src_ref=out_buf.at[peer],
            dst_ref=in_buf.at[sp],
            send_sem=x_send,
            recv_sem=x_recv,
            device_id=(peer, tp),
            device_id_type=MESH,
        ).start()
    pltpu.make_async_copy(
        in_buf.at[pl.ds(0, groups - 1)], in_buf.at[pl.ds(0, groups - 1)], x_recv
    ).wait()
    in_buf[sp] = out_buf[sp]
    whole = in_buf[0]
    for d in range(1, groups):
        whole = whole + in_buf[d]

    for p in range(3):
        rows = whole[p * 4 : p * 4 + 4, :].astype(jnp.bfloat16)
        state_ref[p, 0] = rows[:, 0:HD]
        state_ref[p, 1] = rows[:, HD:]
    raw = whole[12:15, :] + own_term[0:3, :]
    centered = raw - head_sums(raw) * (1.0 / HD)
    scale = lax.rsqrt(head_sums(centered * centered) * (1.0 / HD) + 1e-05)
    read_ref[...] = (centered * scale).astype(jnp.bfloat16)

    def drain(view, sem):
        pltpu.make_async_copy(view, view, sem).wait()

    drain(blocks.at[pl.ds(0, STEPS)], up_send)
    drain(blocks.at[pl.ds(0, STEPS)], dn_send)
    drain(blocks.at[pl.ds(0, 2 * STEPS + NCH)], pt_send)
    for k in range(8):
        drain(news.at[0], nu_send.at[k])
    for k in range(7):
        drain(news.at[0], nd_send.at[k])
    for k in range(16):
        drain(news.at[0], np_send.at[k])
    drain(in_buf.at[pl.ds(0, groups - 1)], x_send)


def body(tokens, new_token, query_weight, key_weight, value_weight, log_decay):
    groups = lax.axis_size("sp")
    n_tp = lax.axis_size("tp")
    depth = n_tp * LANES
    dma = pltpu.SemaphoreType.DMA
    anywhere = pl.BlockSpec(memory_space=pl.ANY)
    vmem = pl.BlockSpec(memory_space=pltpu.VMEM)
    return pl.pallas_call(
        functools.partial(kernel, groups),
        out_shape=(
            jax.ShapeDtypeStruct((3, 2, HD // groups, HD), jnp.bfloat16),
            jax.ShapeDtypeStruct((3, LANES), jnp.bfloat16),
        ),
        in_specs=[
            anywhere,
            vmem,
            anywhere,
            anywhere,
            anywhere,
            pl.BlockSpec(memory_space=pltpu.SMEM),
        ],
        out_specs=(vmem, vmem),
        scratch_shapes=[
            pltpu.VMEM((n_tp * NCH, CH, LANES), jnp.bfloat16),
            pltpu.VMEM((n_tp, 16, LANES), jnp.bfloat16),
            pltpu.VMEM((depth, 3 * LANES), jnp.bfloat16),
            pltpu.VMEM((NCH * CH, 2 * LANES), jnp.float32),
            pltpu.VMEM((16, 3 * LANES), jnp.float32),
            pltpu.VMEM((2 * CH, LANES), jnp.float32),
            pltpu.VMEM((2 * CH, LANES), jnp.float32),
            pltpu.VMEM((2 * CH, LANES), jnp.float32),
            pltpu.VMEM((groups, 16, LANES), jnp.float32),
            pltpu.VMEM((groups, 16, LANES), jnp.float32),
            dma((NCH,)),
            dma((3,)),
            dma,
            dma,
            dma,
            dma((STEPS,)),
            dma((STEPS,)),
            dma((STEPS,)),
            dma((STEPS,)),
            dma((NCH,)),
            dma((8,)),
            dma((7,)),
            dma((16,)),
            dma((8,)),
            dma((7,)),
            dma((8,)),
            dma((7,)),
            dma,
            dma,
            dma,
        ],
        compiler_params=pltpu.CompilerParams(
            collective_id=0, has_side_effects=True, vmem_limit_bytes=48 * 1024 * 1024
        ),
    )(tokens, new_token, query_weight, key_weight, value_weight, log_decay)


def solution(mesh):
    return jax.shard_map(
        body,
        mesh=mesh,
        in_specs=(
            P(None, "sp", "tp"),
            P(None, None, "tp"),
            P(None, "tp"),
            P(None, "tp"),
            P(None, "tp"),
            P("tp"),
        ),
        out_specs=(P(None, "tp", "sp", None), P(None, "tp")),
        check_vma=False,
    )
```

```python
import functools

import jax
import jax.numpy as jnp
import numpy as np
from jax import lax
from jax.experimental import pallas as pl
from jax.experimental.pallas import tpu as pltpu
from jax.sharding import PartitionSpec as P

HD = 64
MESH = pl.DeviceIdType.MESH
NZ = 16
CH = 256
NCH = 6
HALF = 3
STEPS = 7 * NCH + HALF
LANES = 128


def kernel(
    groups,
    tok_ref,
    new_ref,
    wq_ref,
    wk_ref,
    wv_ref,
    ld_ref,
    state_ref,
    read_ref,
    blocks,
    news,
    weights,
    acc,
    acc_new,
    cos_t,
    sin_t,
    dec_t,
    out_buf,
    in_buf,
    tok_sem,
    w_sem,
    up_send,
    dn_send,
    pt_send,
    up_recv,
    dn_recv,
    pu_recv,
    pd_recv,
    own_recv,
    nu_send,
    nd_send,
    np_send,
    nu_recv,
    nd_recv,
    npu_recv,
    npd_recv,
    nown_recv,
    x_send,
    x_recv,
):
    sp = lax.axis_index("sp")
    tp = lax.axis_index("tp")
    z = tp // 2
    core = tp % 2
    up = ((z + 1) % NZ) * 2 + core
    dn = ((z + NZ - 1) % NZ) * 2 + core
    partner = z * 2 + (1 - core)
    span = NCH // 3 * CH

    own_copies = []
    for ch in range(NCH):
        half, p = ch // 3, ch % 3
        c = pltpu.make_async_copy(
            tok_ref.at[p, pl.ds(half * CH, CH), :], blocks.at[tp * NCH + ch], tok_sem.at[ch]
        )
        c.start()
        own_copies.append(c)
    w_copies = []
    for i, ref in enumerate((wk_ref, wv_ref, wq_ref)):
        c = pltpu.make_async_copy(ref, weights.at[:, pl.ds(i * LANES, LANES)], w_sem.at[i])
        c.start()
        w_copies.append(c)

    barrier = pltpu.get_barrier_semaphore()
    for peer in (up, dn, partner):
        pl.semaphore_signal(barrier, inc=1, device_id=(sp, peer), device_id_type=MESH)
    for d in range(1, groups):
        pl.semaphore_signal(
            barrier, inc=1, device_id=((sp + d) % groups, tp), device_id_type=MESH
        )

    own_new = jnp.concatenate(
        [new_ref[...].astype(jnp.float32), jnp.zeros((13, LANES), jnp.float32)], axis=0
    )
    news[tp] = own_new.astype(jnp.bfloat16)

    pl.semaphore_wait(barrier, 3 + groups - 1)

    def remote(src, send, recv, peer, ref=None):
        ref = blocks if ref is None else ref
        return pltpu.make_async_remote_copy(
            src_ref=ref.at[src],
            dst_ref=ref.at[src],
            send_sem=send,
            recv_sem=recv,
            device_id=(sp, peer),
            device_id_type=MESH,
        )

    remote(tp, nu_send.at[0], nu_recv.at[0], up, news).start()
    remote(tp, nd_send.at[0], nd_recv.at[0], dn, news).start()
    remote(tp, np_send.at[15], nown_recv, partner, news).start()
    for ch in range(NCH):
        own_copies[ch].wait()
    for pos in range(NCH):
        cu, cd = pos, (pos + HALF) % NCH
        remote(tp * NCH + cu, up_send, up_recv.at[pos], up).start()
        remote(tp * NCH + cd, dn_send, dn_recv.at[pos], dn).start()
    for ch in range(NCH):
        remote(tp * NCH + ch, pt_send, own_recv.at[ch], partner).start()

    def source(t, down):
        k, pos = t // NCH, t % NCH
        if down:
            sz = (z + 1 + k) % NZ
            ch = (pos + HALF) % NCH
        else:
            sz = (z + NZ - 1 - k) % NZ
            ch = pos
        return k, sz, ch

    lane = lax.broadcasted_iota(jnp.int32, (1, LANES), 1)
    inverse = jnp.zeros((1, LANES), jnp.float32)
    freq = (10000.0 ** (-np.arange(32, dtype=np.float64) / 32)).astype(np.float32)
    for i in range(32):
        inverse = jnp.where(lane % 32 == i, float(freq[i]), inverse)
    first = (lane % HD) < 32
    low = lane < HD
    ld = jnp.where(low, ld_ref[0], ld_ref[1])
    row = lax.broadcasted_iota(jnp.int32, (span, LANES), 0)
    angle = (row + sp * span).astype(jnp.float32) * inverse
    cos_t[...] = jnp.cos(angle) * 0.125
    sin_t[...] = jnp.where(first, -jnp.sin(angle), jnp.sin(angle)) * 0.125
    dec_t[...] = jnp.exp((span - 1 - row).astype(jnp.float32) * ld)
    carried = jnp.exp(ld * (span * (groups - 1 - sp)).astype(jnp.float32))

    for c in w_copies:
        c.wait()

    def lhs(sz, ch):
        return jnp.concatenate(
            [blocks[(2 * sz) * NCH + ch], blocks[(2 * sz + 1) * NCH + ch]], axis=1
        )

    def rows_of(sz):
        return pl.ds(pl.multiple_of(sz * 256, 256), 256)

    def new_dot(sz):
        x = jnp.concatenate([news[2 * sz], news[2 * sz + 1]], axis=1)
        return jnp.dot(x, weights[rows_of(sz), :], preferred_element_type=jnp.float32)

    def kv_dot(sz, ch):
        return jnp.dot(
            lhs(sz, ch), weights[rows_of(sz), 0:256], preferred_element_type=jnp.float32
        )

    remote(partner, np_send.at[15], nown_recv, partner, news).wait_recv()
    acc_new[...] = new_dot(z)
    for ch in range(NCH):
        remote(partner * NCH + ch, pt_send, own_recv.at[ch], partner).wait_recv()
        acc[pl.ds(ch * CH, CH), :] = kv_dot(z, ch)

    def relay(t):
        k, su, cu = source(t, False)
        _, sd, cd = source(t, True)
        bu = (su * 2 + core) * NCH + cu
        bd = (sd * 2 + core) * NCH + cd

        def small():
            nu = su * 2 + core
            nd = sd * 2 + core
            remote(nu, nu_send.at[k], nu_recv.at[k], up, news).wait_recv()

            @pl.when(k < 7)
            def _():
                remote(nu, nu_send.at[k + 1], nu_recv.at[k + 1], up, news).start()
                remote(nd, nd_send.at[k], nd_recv.at[k], dn, news).wait_recv()

                @pl.when(k < 6)
                def _():
                    remote(nd, nd_send.at[k + 1], nd_recv.at[k + 1], dn, news).start()

                remote(nd, np_send.at[k + 8], npd_recv.at[k], partner, news).start()

            remote(nu, np_send.at[k], npu_recv.at[k], partner, news).start()

        if isinstance(t, int):
            if t % NCH == 0:
                small()
        else:
            pl.when(t % NCH == 0)(small)

        def forward():
            remote(bu, up_send, up_recv.at[t + NCH], up).start()

        def forward_down():
            remote(bd, dn_send, dn_recv.at[t + NCH], dn).start()

        remote(bu, up_send, up_recv.at[t], up).wait_recv()
        if isinstance(t, int):
            if t + NCH < STEPS:
                forward()
        else:
            pl.when(t + NCH < STEPS)(forward)
        remote(bu, pt_send, pu_recv.at[t], partner).start()
        remote(bd, dn_send, dn_recv.at[t], dn).wait_recv()
        if isinstance(t, int):
            if t + NCH < STEPS:
                forward_down()
        else:
            pl.when(t + NCH < STEPS)(forward_down)
        remote(bd, pt_send, pd_recv.at[t], partner).start()

    def compute(t):
        k, su, cu = source(t, False)
        _, sd, cd = source(t, True)
        pc = 1 - core

        def small():
            remote(su * 2 + pc, np_send.at[k], npu_recv.at[k], partner, news).wait_recv()
            acc_new[...] += new_dot(su)

            @pl.when(k < 7)
            def _():
                remote(sd * 2 + pc, np_send.at[k], npd_recv.at[k], partner, news).wait_recv()
                acc_new[...] += new_dot(sd)

        if isinstance(t, int):
            if t % NCH == 0:
                small()
        else:
            pl.when(t % NCH == 0)(small)
        remote((su * 2 + pc) * NCH + cu, pt_send, pu_recv.at[t], partner).wait_recv()
        at = pl.ds(pl.multiple_of(cu * CH, CH), CH)
        acc[at, :] += kv_dot(su, cu)
        remote((sd * 2 + pc) * NCH + cd, pt_send, pd_recv.at[t], partner).wait_recv()
        at = pl.ds(pl.multiple_of(cd * CH, CH), CH)
        acc[at, :] += kv_dot(sd, cd)

    last = STEPS - HALF

    def step(t, carry):
        relay(t)
        pl.when(t >= 1)(lambda: compute(t - 1))
        return carry

    lax.fori_loop(0, last + 1, step, 0)

    def turned(x, cosine, sine):
        swapped = jnp.where(first, pltpu.roll(x, LANES - 32, 1), pltpu.roll(x, 32, 1))
        return x * cosine + swapped * sine

    relay(last + 1)
    compute(last)

    new_angle = (groups * span) * inverse
    new_cos = jnp.cos(new_angle)
    new_sin = jnp.where(first, -jnp.sin(new_angle), jnp.sin(new_angle))
    new_k = (turned(acc_new[0:8, 0:128], new_cos, new_sin) * 0.125).astype(jnp.bfloat16)
    new_v = acc_new[0:8, 128:256].astype(jnp.bfloat16).astype(jnp.float32)
    new_q = turned(acc_new[0:8, 256:384], new_cos, new_sin).astype(jnp.bfloat16)
    new_q = new_q.astype(jnp.float32)
    product = new_q * new_k.astype(jnp.float32)

    def head_sums(x):
        lo = jnp.sum(jnp.where(low, x, 0.0), axis=1, keepdims=True)
        hi = jnp.sum(jnp.where(low, 0.0, x), axis=1, keepdims=True)
        return jnp.where(low, lo, hi)

    own_term = head_sums(product) * new_v
    q_cols = jnp.transpose(jnp.concatenate([new_q] * 16, axis=0))
    one = jnp.exp(ld)

    def finish(p):
        total = None
        for half in range(2):
            at = pl.ds(half * CH, CH)
            rows = acc[pl.ds((half * 3 + p) * CH, CH), :]
            keys = turned(rows[:, 0:128], cos_t[at, :], sin_t[at, :]).astype(jnp.bfloat16)
            keys = (keys.astype(jnp.float32) * dec_t[at, :]).astype(jnp.bfloat16)
            part = lax.dot_general(
                keys,
                rows[:, 128:256].astype(jnp.bfloat16),
                (((0,), (0,)), ((), ())),
                preferred_element_type=jnp.float32,
            )
            total = part if total is None else total + part
        tile = jnp.where(low, total[0:HD, :], total[HD:, :]) * carried
        query = jnp.where(low, q_cols[0:HD, p : p + 1], q_cols[HD:, p : p + 1])
        partial = jnp.sum(tile * query, axis=0, keepdims=True) * one
        out_buf[p, :, pl.ds(0, 4), :] = tile.reshape(groups, HD // groups, LANES)
        out_buf[p, :, pl.ds(4, 1), :] = jnp.broadcast_to(partial[None], (groups, 1, LANES))
        in_buf[p, sp] = out_buf[p, sp]
        for d in range(1, groups):
            peer = (sp + d) % groups
            pltpu.make_async_remote_copy(
                src_ref=out_buf.at[p, peer],
                dst_ref=in_buf.at[p, sp],
                send_sem=x_send.at[p],
                recv_sem=x_recv.at[p],
                device_id=(peer, tp),
                device_id_type=MESH,
            ).start()

    def arrived(p):
        view = in_buf.at[p, pl.ds(0, groups - 1)]
        pltpu.make_async_copy(view, view, x_recv.at[p]).wait()
        parts = [in_buf[p, d] for d in range(groups)]
        while len(parts) > 1:
            parts = [parts[i] + parts[i + 1] for i in range(0, len(parts), 2)]
        whole = parts[0]
        rows = whole[0:4, :].astype(jnp.bfloat16)
        state_ref[p, 0] = rows[:, 0:HD]
        state_ref[p, 1] = rows[:, HD:]
        raw = whole[4:5, :] + own_term[p : p + 1, :]
        centered = raw - head_sums(raw) * (1.0 / HD)
        scale = lax.rsqrt(head_sums(centered * centered) * (1.0 / HD) + 1e-05)
        read_ref[pl.ds(p, 1), :] = (centered * scale).astype(jnp.bfloat16)

    out_buf[:, :, pl.ds(5, 3), :] = jnp.zeros((3, groups, 3, LANES), jnp.float32)
    finish(0)
    relay(last + 2)
    compute(last + 1)
    finish(1)
    compute(last + 2)
    finish(2)
    for p in range(3):
        arrived(p)

    def drain(view, sem):
        pltpu.make_async_copy(view, view, sem).wait()

    drain(blocks.at[pl.ds(0, STEPS)], up_send)
    drain(blocks.at[pl.ds(0, STEPS)], dn_send)
    drain(blocks.at[pl.ds(0, 2 * STEPS + NCH)], pt_send)
    for k in range(8):
        drain(news.at[0], nu_send.at[k])
    for k in range(7):
        drain(news.at[0], nd_send.at[k])
    for k in range(16):
        drain(news.at[0], np_send.at[k])
    for p in range(3):
        drain(in_buf.at[p, pl.ds(0, groups - 1)], x_send.at[p])


def body(tokens, new_token, query_weight, key_weight, value_weight, log_decay):
    groups = lax.axis_size("sp")
    n_tp = lax.axis_size("tp")
    depth = n_tp * LANES
    dma = pltpu.SemaphoreType.DMA
    anywhere = pl.BlockSpec(memory_space=pltpu.HBM)
    vmem = pl.BlockSpec(memory_space=pltpu.VMEM)
    return pl.pallas_call(
        functools.partial(kernel, groups),
        out_shape=(
            jax.ShapeDtypeStruct((3, 2, HD // groups, HD), jnp.bfloat16),
            jax.ShapeDtypeStruct((3, LANES), jnp.bfloat16),
        ),
        in_specs=[
            anywhere,
            vmem,
            anywhere,
            anywhere,
            anywhere,
            pl.BlockSpec(memory_space=pltpu.SMEM),
        ],
        out_specs=(vmem, vmem),
        scratch_shapes=[
            pltpu.VMEM((n_tp * NCH, CH, LANES), jnp.bfloat16),
            pltpu.VMEM((n_tp, 16, LANES), jnp.bfloat16),
            pltpu.VMEM((depth, 3 * LANES), jnp.bfloat16),
            pltpu.VMEM((NCH * CH, 2 * LANES), jnp.float32),
            pltpu.VMEM((16, 3 * LANES), jnp.float32),
            pltpu.VMEM((2 * CH, LANES), jnp.float32),
            pltpu.VMEM((2 * CH, LANES), jnp.float32),
            pltpu.VMEM((2 * CH, LANES), jnp.float32),
            pltpu.VMEM((3, groups, 8, LANES), jnp.float32),
            pltpu.VMEM((3, groups, 8, LANES), jnp.float32),
            dma((NCH,)),
            dma((3,)),
            dma,
            dma,
            dma,
            dma((STEPS,)),
            dma((STEPS,)),
            dma((STEPS,)),
            dma((STEPS,)),
            dma((NCH,)),
            dma((8,)),
            dma((7,)),
            dma((16,)),
            dma((8,)),
            dma((7,)),
            dma((8,)),
            dma((7,)),
            dma,
            dma((3,)),
            dma((3,)),
        ],
        compiler_params=pltpu.CompilerParams(
            collective_id=0, has_side_effects=True, vmem_limit_bytes=55112 * 1024
        ),
    )(tokens, new_token[:, 0, :], query_weight, key_weight, value_weight, log_decay)


def solution(mesh):
    return jax.shard_map(
        body,
        mesh=mesh,
        in_specs=(
            P(None, "sp", "tp"),
            P(None, None, "tp"),
            P(None, "tp"),
            P(None, "tp"),
            P(None, "tp"),
            P("tp"),
        ),
        out_specs=(P(None, "tp", "sp", None), P(None, "tp")),
        check_vma=False,
    )
```

```python
import functools

import jax
import jax.numpy as jnp
import numpy as np
from jax import lax
from jax.experimental import pallas as pl
from jax.experimental.pallas import tpu as pltpu
from jax.sharding import PartitionSpec as P

HD = 64
MESH = pl.DeviceIdType.MESH
NZ = 16
CH = 256
NCH = 6
HALF = 3
STEPS = 7 * NCH + HALF
LANES = 128


def kernel(
    groups,
    tok_ref,
    new_ref,
    wq_ref,
    wk_ref,
    wv_ref,
    ld_ref,
    state_ref,
    read_ref,
    blocks,
    news,
    weights,
    acc,
    acc_new,
    cos_t,
    sin_t,
    dec_t,
    out_buf,
    in_buf,
    tok_sem,
    w_sem,
    up_send,
    dn_send,
    pt_send,
    up_recv,
    dn_recv,
    pu_recv,
    pd_recv,
    own_recv,
    nu_send,
    nd_send,
    np_send,
    nu_recv,
    nd_recv,
    npu_recv,
    npd_recv,
    nown_recv,
    x_send,
    x_recv,
    ready,
):
    sp = lax.axis_index("sp")
    tp = lax.axis_index("tp")
    z = tp // 2
    y, x = sp // 4, sp % 4
    core = tp % 2
    up = ((z + 1) % NZ) * 2 + core
    dn = ((z + NZ - 1) % NZ) * 2 + core
    partner = z * 2 + (1 - core)
    span = NCH // 3 * CH

    own_copies = []
    for ch in range(NCH):
        half, p = ch // 3, ch % 3
        c = pltpu.make_async_copy(
            tok_ref.at[p, pl.ds(half * CH, CH), :], blocks.at[tp * NCH + ch], tok_sem.at[ch]
        )
        c.start()
        own_copies.append(c)
    w_copies = []
    for i, ref in enumerate((wk_ref, wv_ref, wq_ref)):
        c = pltpu.make_async_copy(ref, weights.at[:, pl.ds(i * LANES, LANES)], w_sem.at[i])
        c.start()
        w_copies.append(c)

    barrier = pltpu.get_barrier_semaphore()
    for peer in (up, dn, partner):
        pl.semaphore_signal(barrier, inc=1, device_id=(sp, peer), device_id_type=MESH)
    beside = [y * 4 + (x + d) % 4 for d in (1, 3)] + [((y + d) % 4) * 4 + x for d in (1, 3)]
    for peer in beside:
        pl.semaphore_signal(barrier, inc=1, device_id=(peer, tp), device_id_type=MESH)

    own_new = jnp.concatenate(
        [new_ref[...].astype(jnp.float32), jnp.zeros((5, LANES), jnp.float32)], axis=0
    )
    news[tp] = own_new.astype(jnp.bfloat16)

    pl.semaphore_wait(barrier, 3 + 4)

    def tell(r):
        for peer in beside:
            pl.semaphore_signal(ready.at[r], inc=1, device_id=(peer, tp), device_id_type=MESH)

    def told(r):
        pl.semaphore_wait(ready.at[r], 4)

    tell(0)

    def remote(src, send, recv, peer, ref=None):
        ref = blocks if ref is None else ref
        return pltpu.make_async_remote_copy(
            src_ref=ref.at[src],
            dst_ref=ref.at[src],
            send_sem=send,
            recv_sem=recv,
            device_id=(sp, peer),
            device_id_type=MESH,
        )

    remote(tp, nu_send.at[0], nu_recv.at[0], up, news).start()
    remote(tp, nd_send.at[0], nd_recv.at[0], dn, news).start()
    remote(tp, np_send.at[15], nown_recv, partner, news).start()
    for ch in range(NCH):
        own_copies[ch].wait()
    for pos in range(NCH):
        cu, cd = pos, (pos + HALF) % NCH
        remote(tp * NCH + cu, up_send, up_recv.at[pos], up).start()
        remote(tp * NCH + cd, dn_send, dn_recv.at[pos], dn).start()
    for ch in range(NCH):
        remote(tp * NCH + ch, pt_send, own_recv.at[ch], partner).start()

    def source(t, down):
        k, pos = t // NCH, t % NCH
        if down:
            sz = (z + 1 + k) % NZ
            ch = (pos + HALF) % NCH
        else:
            sz = (z + NZ - 1 - k) % NZ
            ch = pos
        return k, sz, ch

    lane = lax.broadcasted_iota(jnp.int32, (1, LANES), 1)
    inverse = jnp.zeros((1, LANES), jnp.float32)
    freq = (10000.0 ** (-np.arange(32, dtype=np.float64) / 32)).astype(np.float32)
    for i in range(32):
        inverse = jnp.where(lane % 32 == i, float(freq[i]), inverse)
    first = (lane % HD) < 32
    low = lane < HD
    ld = jnp.where(low, ld_ref[0], ld_ref[1])
    row = lax.broadcasted_iota(jnp.int32, (span, LANES), 0)
    angle = (row + sp * span).astype(jnp.float32) * inverse
    cos_t[...] = jnp.cos(angle) * 0.125
    sin_t[...] = jnp.where(first, -jnp.sin(angle), jnp.sin(angle)) * 0.125
    dec_t[...] = jnp.exp((span - 1 - row).astype(jnp.float32) * ld)
    carried = jnp.exp(ld * (span * (groups - 1 - sp)).astype(jnp.float32))

    told(0)
    tell(1)
    for c in w_copies:
        c.wait()

    def lhs(sz, ch):
        return jnp.concatenate(
            [blocks[(2 * sz) * NCH + ch], blocks[(2 * sz + 1) * NCH + ch]], axis=1
        )

    def rows_of(sz):
        return pl.ds(pl.multiple_of(sz * 256, 256), 256)

    def new_dot(sz):
        x = jnp.concatenate([news[2 * sz], news[2 * sz + 1]], axis=1)
        return jnp.dot(x, weights[rows_of(sz), :], preferred_element_type=jnp.float32)

    def kv_dot(sz, ch):
        return jnp.dot(
            lhs(sz, ch), weights[rows_of(sz), 0:256], preferred_element_type=jnp.float32
        )

    remote(partner, np_send.at[15], nown_recv, partner, news).wait_recv()
    acc_new[...] = new_dot(z)
    for ch in range(NCH):
        remote(partner * NCH + ch, pt_send, own_recv.at[ch], partner).wait_recv()
        acc[pl.ds(ch * CH, CH), :] = kv_dot(z, ch)

    told(1)
    tell(2)

    def relay(t):
        k, su, cu = source(t, False)
        _, sd, cd = source(t, True)
        bu = (su * 2 + core) * NCH + cu
        bd = (sd * 2 + core) * NCH + cd

        def small():
            nu = su * 2 + core
            nd = sd * 2 + core
            remote(nu, nu_send.at[k], nu_recv.at[k], up, news).wait_recv()

            @pl.when(k < 7)
            def _():
                remote(nu, nu_send.at[k + 1], nu_recv.at[k + 1], up, news).start()
                remote(nd, nd_send.at[k], nd_recv.at[k], dn, news).wait_recv()

                @pl.when(k < 6)
                def _():
                    remote(nd, nd_send.at[k + 1], nd_recv.at[k + 1], dn, news).start()

                remote(nd, np_send.at[k + 8], npd_recv.at[k], partner, news).start()

            remote(nu, np_send.at[k], npu_recv.at[k], partner, news).start()

        if isinstance(t, int):
            if t % NCH == 0:
                small()
        else:
            pl.when(t % NCH == 0)(small)

        def forward():
            remote(bu, up_send, up_recv.at[t + NCH], up).start()

        def forward_down():
            remote(bd, dn_send, dn_recv.at[t + NCH], dn).start()

        remote(bu, up_send, up_recv.at[t], up).wait_recv()
        if isinstance(t, int):
            if t + NCH < STEPS:
                forward()
        else:
            pl.when(t + NCH < STEPS)(forward)
        remote(bu, pt_send, pu_recv.at[t], partner).start()
        remote(bd, dn_send, dn_recv.at[t], dn).wait_recv()
        if isinstance(t, int):
            if t + NCH < STEPS:
                forward_down()
        else:
            pl.when(t + NCH < STEPS)(forward_down)
        remote(bd, pt_send, pd_recv.at[t], partner).start()

    def compute(t):
        k, su, cu = source(t, False)
        _, sd, cd = source(t, True)
        pc = 1 - core

        def small():
            remote(su * 2 + pc, np_send.at[k], npu_recv.at[k], partner, news).wait_recv()
            acc_new[...] += new_dot(su)

            @pl.when(k < 7)
            def _():
                remote(sd * 2 + pc, np_send.at[k], npd_recv.at[k], partner, news).wait_recv()
                acc_new[...] += new_dot(sd)

        if isinstance(t, int):
            if t % NCH == 0:
                small()
        else:
            pl.when(t % NCH == 0)(small)
        remote((su * 2 + pc) * NCH + cu, pt_send, pu_recv.at[t], partner).wait_recv()
        at = pl.ds(pl.multiple_of(cu * CH, CH), CH)
        acc[at, :] += kv_dot(su, cu)
        remote((sd * 2 + pc) * NCH + cd, pt_send, pd_recv.at[t], partner).wait_recv()
        at = pl.ds(pl.multiple_of(cd * CH, CH), CH)
        acc[at, :] += kv_dot(sd, cd)

    last = STEPS - HALF

    def step(t, carry):
        relay(t)
        pl.when(t >= 1)(lambda: compute(t - 1))
        return carry

    lax.fori_loop(0, last + 1, step, 0)

    def turned(x, cosine, sine):
        swapped = jnp.where(first, pltpu.roll(x, LANES - 32, 1), pltpu.roll(x, 32, 1))
        return x * cosine + swapped * sine

    told(2)
    relay(last + 1)
    compute(last)

    new_angle = (groups * span) * inverse
    new_cos = jnp.cos(new_angle)
    new_sin = jnp.where(first, -jnp.sin(new_angle), jnp.sin(new_angle))
    new_k = (turned(acc_new[0:8, 0:128], new_cos, new_sin) * 0.125).astype(jnp.bfloat16)
    new_v = acc_new[0:8, 128:256].astype(jnp.bfloat16).astype(jnp.float32)
    new_q = turned(acc_new[0:8, 256:384], new_cos, new_sin).astype(jnp.bfloat16)
    new_q = new_q.astype(jnp.float32)
    product = new_q * new_k.astype(jnp.float32)

    def head_sums(x):
        lo = jnp.sum(jnp.where(low, x, 0.0), axis=1, keepdims=True)
        hi = jnp.sum(jnp.where(low, 0.0, x), axis=1, keepdims=True)
        return jnp.where(low, lo, hi)

    own_term = head_sums(product) * new_v
    q_cols = jnp.transpose(jnp.concatenate([new_q] * 16, axis=0))
    one = jnp.exp(ld)

    def finish(p):
        total = None
        for half in range(2):
            at = pl.ds(half * CH, CH)
            rows = acc[pl.ds((half * 3 + p) * CH, CH), :]
            keys = turned(rows[:, 0:128], cos_t[at, :], sin_t[at, :]).astype(jnp.bfloat16)
            keys = (keys.astype(jnp.float32) * dec_t[at, :]).astype(jnp.bfloat16)
            part = lax.dot_general(
                keys,
                rows[:, 128:256].astype(jnp.bfloat16),
                (((0,), (0,)), ((), ())),
                preferred_element_type=jnp.float32,
            )
            total = part if total is None else total + part
        tile = jnp.where(low, total[0:HD, :], total[HD:, :]) * carried
        query = jnp.where(low, q_cols[0:HD, p : p + 1], q_cols[HD:, p : p + 1])
        partial = jnp.sum(tile * query, axis=0, keepdims=True) * one
        packed = [
            tile.reshape(groups, HD // groups, LANES),
            jnp.broadcast_to(partial[None], (groups, 1, LANES)),
            jnp.zeros((groups, 3, LANES), jnp.float32),
        ]
        out_buf[p] = jnp.concatenate(packed, axis=1).astype(jnp.bfloat16)
        in_buf[p, sp] = out_buf[p, sp]
        for d in range(1, groups):
            peer = (sp + d) % groups
            pltpu.make_async_remote_copy(
                src_ref=out_buf.at[p, peer],
                dst_ref=in_buf.at[p, sp],
                send_sem=x_send.at[p],
                recv_sem=x_recv.at[p],
                device_id=(peer, tp),
                device_id_type=MESH,
            ).start()

    def arrived(p):
        view = in_buf.at[p, pl.ds(0, groups - 1)]
        pltpu.make_async_copy(view, view, x_recv.at[p]).wait()
        parts = [in_buf[p, d].astype(jnp.float32) for d in range(groups)]
        while len(parts) > 1:
            parts = [parts[i] + parts[i + 1] for i in range(0, len(parts), 2)]
        whole = parts[0]
        rows = whole[0:4, :].astype(jnp.bfloat16)
        state_ref[p, 0] = rows[:, 0:HD]
        state_ref[p, 1] = rows[:, HD:]
        raw = whole[4:5, :] + own_term[p : p + 1, :]
        centered = raw - head_sums(raw) * (1.0 / HD)
        scale = lax.rsqrt(head_sums(centered * centered) * (1.0 / HD) + 1e-05)
        read_ref[pl.ds(p, 1), :] = (centered * scale).astype(jnp.bfloat16)

    finish(0)
    relay(last + 2)
    compute(last + 1)
    finish(1)
    compute(last + 2)
    finish(2)
    for p in range(3):
        arrived(p)

    def drain(view, sem):
        pltpu.make_async_copy(view, view, sem).wait()

    drain(blocks.at[pl.ds(0, STEPS)], up_send)
    drain(blocks.at[pl.ds(0, STEPS)], dn_send)
    drain(blocks.at[pl.ds(0, 2 * STEPS + NCH)], pt_send)
    for k in range(8):
        drain(news.at[0], nu_send.at[k])
    for k in range(7):
        drain(news.at[0], nd_send.at[k])
    for k in range(16):
        drain(news.at[0], np_send.at[k])
    for p in range(3):
        drain(in_buf.at[p, pl.ds(0, groups - 1)], x_send.at[p])


def body(tokens, new_token, query_weight, key_weight, value_weight, log_decay):
    groups = lax.axis_size("sp")
    n_tp = lax.axis_size("tp")
    depth = n_tp * LANES
    dma = pltpu.SemaphoreType.DMA
    anywhere = pl.BlockSpec(memory_space=pltpu.HBM)
    vmem = pl.BlockSpec(memory_space=pltpu.VMEM)
    return pl.pallas_call(
        functools.partial(kernel, groups),
        out_shape=(
            jax.ShapeDtypeStruct((3, 2, HD // groups, HD), jnp.bfloat16),
            jax.ShapeDtypeStruct((3, LANES), jnp.bfloat16),
        ),
        in_specs=[
            anywhere,
            vmem,
            anywhere,
            anywhere,
            anywhere,
            pl.BlockSpec(memory_space=pltpu.SMEM),
        ],
        out_specs=(vmem, vmem),
        scratch_shapes=[
            pltpu.VMEM((n_tp * NCH, CH, LANES), jnp.bfloat16),
            pltpu.VMEM((n_tp, 8, LANES), jnp.bfloat16),
            pltpu.VMEM((depth, 3 * LANES), jnp.bfloat16),
            pltpu.VMEM((NCH * CH, 2 * LANES), jnp.float32),
            pltpu.VMEM((8, 3 * LANES), jnp.float32),
            pltpu.VMEM((2 * CH, LANES), jnp.float32),
            pltpu.VMEM((2 * CH, LANES), jnp.float32),
            pltpu.VMEM((2 * CH, LANES), jnp.float32),
            pltpu.VMEM((3, groups, 8, LANES), jnp.bfloat16),
            pltpu.VMEM((3, groups, 8, LANES), jnp.bfloat16),
            dma((NCH,)),
            dma((3,)),
            dma,
            dma,
            dma,
            dma((STEPS,)),
            dma((STEPS,)),
            dma((STEPS,)),
            dma((STEPS,)),
            dma((NCH,)),
            dma((8,)),
            dma((7,)),
            dma((16,)),
            dma((8,)),
            dma((7,)),
            dma((8,)),
            dma((7,)),
            dma,
            dma((3,)),
            dma((3,)),
            pltpu.SemaphoreType.REGULAR((3,)),
        ],
        compiler_params=pltpu.CompilerParams(
            collective_id=0, has_side_effects=True, vmem_limit_bytes=55112 * 1024
        ),
    )(tokens, new_token[:, 0, :], query_weight, key_weight, value_weight, log_decay)


def solution(mesh):
    return jax.shard_map(
        body,
        mesh=mesh,
        in_specs=(
            P(None, "sp", "tp"),
            P(None, None, "tp"),
            P(None, "tp"),
            P(None, "tp"),
            P(None, "tp"),
            P("tp"),
        ),
        out_specs=(P(None, "tp", "sp", None), P(None, "tp")),
        check_vma=False,
    )
```

```python
import functools

import jax
import jax.numpy as jnp
import numpy as np
from jax import lax
from jax.experimental import pallas as pl
from jax.experimental.pallas import tpu as pltpu
from jax.sharding import PartitionSpec as P

HD = 64
MESH = pl.DeviceIdType.MESH
NZ = 16
CH = 256
PARTS = 2
NCH = 3 * PARTS
HALF = NCH // 2
STEPS = 7 * NCH + HALF
LANES = 128
OTHERS = sorted(
    ((dy, dx) for dy in range(4) for dx in range(4) if dy or dx),
    key=lambda d: -sum(min(v, 4 - v) for v in d),
)


def kernel(
    groups,
    tok_ref,
    new_ref,
    wq_ref,
    wk_ref,
    wv_ref,
    ld_ref,
    state_ref,
    read_ref,
    blocks,
    news,
    weights,
    acc,
    acc_new,
    cos_t,
    sin_t,
    dec_t,
    out_buf,
    in_buf,
    tok_sem,
    w_sem,
    up_send,
    dn_send,
    pt_send,
    up_recv,
    dn_recv,
    pu_recv,
    pd_recv,
    own_recv,
    nu_send,
    nd_send,
    np_send,
    nu_recv,
    nd_recv,
    npu_recv,
    npd_recv,
    nown_recv,
    x_send,
    x_recv,
    ready,
):
    sp = lax.axis_index("sp")
    tp = lax.axis_index("tp")
    z = tp // 2
    y, x = sp // 4, sp % 4
    core = tp % 2
    up = ((z + 1) % NZ) * 2 + core
    dn = ((z + NZ - 1) % NZ) * 2 + core
    partner = z * 2 + (1 - core)
    span = PARTS * CH

    barrier = pltpu.get_barrier_semaphore()
    for peer in (up, dn, partner):
        pl.semaphore_signal(barrier, inc=1, device_id=(sp, peer), device_id_type=MESH)
    beside = [y * 4 + (x + d) % 4 for d in (1, 3)] + [((y + d) % 4) * 4 + x for d in (1, 3)]
    for peer in beside:
        pl.semaphore_signal(barrier, inc=1, device_id=(peer, tp), device_id_type=MESH)

    own_copies = []
    for ch in range(NCH):
        part, p = ch // 3, ch % 3
        c = pltpu.make_async_copy(
            tok_ref.at[p, pl.ds(part * CH, CH), :], blocks.at[tp * NCH + ch], tok_sem.at[ch]
        )
        c.start()
        own_copies.append(c)
    w_copies = []
    for i, ref in enumerate((wk_ref, wv_ref, wq_ref)):
        c = pltpu.make_async_copy(ref, weights.at[:, pl.ds(i * LANES, LANES)], w_sem.at[i])
        c.start()
        w_copies.append(c)

    own_new = jnp.concatenate(
        [new_ref[...].astype(jnp.float32), jnp.zeros((5, LANES), jnp.float32)], axis=0
    )
    news[tp] = own_new.astype(jnp.bfloat16)

    pl.semaphore_wait(barrier, 3 + 4)

    def tell(r):
        for peer in beside:
            pl.semaphore_signal(ready.at[r], inc=1, device_id=(peer, tp), device_id_type=MESH)

    def told(r):
        pl.semaphore_wait(ready.at[r], 4)

    tell(0)

    def remote(src, send, recv, peer, ref=None):
        ref = blocks if ref is None else ref
        return pltpu.make_async_remote_copy(
            src_ref=ref.at[src],
            dst_ref=ref.at[src],
            send_sem=send,
            recv_sem=recv,
            device_id=(sp, peer),
            device_id_type=MESH,
        )

    remote(tp, nu_send.at[0], nu_recv.at[0], up, news).start()
    remote(tp, nd_send.at[0], nd_recv.at[0], dn, news).start()
    remote(tp, np_send.at[15], nown_recv, partner, news).start()
    for pos in range(NCH):
        cu, cd = pos, (pos + HALF) % NCH
        if pos < HALF:
            own_copies[cu].wait()
            own_copies[cd].wait()
        remote(tp * NCH + cu, up_send, up_recv.at[pos], up).start()
        remote(tp * NCH + cd, dn_send, dn_recv.at[pos], dn).start()
    for ch in range(NCH):
        remote(tp * NCH + ch, pt_send, own_recv.at[ch], partner).start()

    def source(t, down):
        k, pos = t // NCH, t % NCH
        if down:
            sz = (z + 1 + k) % NZ
            ch = (pos + HALF) % NCH
        else:
            sz = (z + NZ - 1 - k) % NZ
            ch = pos
        return k, sz, ch

    lane = lax.broadcasted_iota(jnp.int32, (1, LANES), 1)
    inverse = jnp.zeros((1, LANES), jnp.float32)
    freq = (10000.0 ** (-np.arange(32, dtype=np.float64) / 32)).astype(np.float32)
    for i in range(32):
        inverse = jnp.where(lane % 32 == i, float(freq[i]), inverse)
    first = (lane % HD) < 32
    low = lane < HD
    ld = jnp.where(low, ld_ref[0:1, 0:1], ld_ref[0:1, 1:2])
    row = lax.broadcasted_iota(jnp.int32, (span, LANES), 0)
    angle = (row + sp * span).astype(jnp.float32) * inverse
    cos_t[...] = jnp.cos(angle) * 0.125
    sin_t[...] = jnp.where(first, -jnp.sin(angle), jnp.sin(angle)) * 0.125
    dec_t[...] = jnp.exp((span - 1 - row).astype(jnp.float32) * ld)
    carried = jnp.exp(ld * (span * (groups - 1 - sp)).astype(jnp.float32))

    told(0)
    tell(1)
    for c in w_copies:
        c.wait()

    def lhs(sz, ch):
        return jnp.concatenate(
            [blocks[(2 * sz) * NCH + ch], blocks[(2 * sz + 1) * NCH + ch]], axis=1
        )

    def rows_of(sz):
        return pl.ds(pl.multiple_of(sz * 256, 256), 256)

    def new_dot(sz):
        x = jnp.concatenate([news[2 * sz], news[2 * sz + 1]], axis=1)
        return jnp.dot(x, weights[rows_of(sz), :], preferred_element_type=jnp.float32)

    def kv_dot(sz, ch):
        return jnp.dot(
            lhs(sz, ch), weights[rows_of(sz), 0:256], preferred_element_type=jnp.float32
        )

    remote(partner, np_send.at[15], nown_recv, partner, news).wait_recv()
    acc_new[...] = new_dot(z)
    for ch in range(NCH):
        remote(partner * NCH + ch, pt_send, own_recv.at[ch], partner).wait_recv()
        acc[pl.ds(ch * CH, CH), :] = kv_dot(z, ch)

    told(1)
    tell(2)

    def relay(t):
        k, su, cu = source(t, False)
        _, sd, cd = source(t, True)
        bu = (su * 2 + core) * NCH + cu
        bd = (sd * 2 + core) * NCH + cd

        def small():
            nu = su * 2 + core
            nd = sd * 2 + core
            remote(nu, nu_send.at[k], nu_recv.at[k], up, news).wait_recv()

            @pl.when(k < 7)
            def _():
                remote(nu, nu_send.at[k + 1], nu_recv.at[k + 1], up, news).start()
                remote(nd, nd_send.at[k], nd_recv.at[k], dn, news).wait_recv()

                @pl.when(k < 6)
                def _():
                    remote(nd, nd_send.at[k + 1], nd_recv.at[k + 1], dn, news).start()

                remote(nd, np_send.at[k + 8], npd_recv.at[k], partner, news).start()

            remote(nu, np_send.at[k], npu_recv.at[k], partner, news).start()

        if isinstance(t, int):
            if t % NCH == 0:
                small()
        else:
            pl.when(t % NCH == 0)(small)

        def forward():
            remote(bu, up_send, up_recv.at[t + NCH], up).start()

        def forward_down():
            remote(bd, dn_send, dn_recv.at[t + NCH], dn).start()

        remote(bu, up_send, up_recv.at[t], up).wait_recv()
        if isinstance(t, int):
            if t + NCH < STEPS:
                forward()
        else:
            pl.when(t + NCH < STEPS)(forward)
        remote(bu, pt_send, pu_recv.at[t], partner).start()
        remote(bd, dn_send, dn_recv.at[t], dn).wait_recv()
        if isinstance(t, int):
            if t + NCH < STEPS:
                forward_down()
        else:
            pl.when(t + NCH < STEPS)(forward_down)
        remote(bd, pt_send, pd_recv.at[t], partner).start()

    def compute(t):
        k, su, cu = source(t, False)
        _, sd, cd = source(t, True)
        pc = 1 - core

        def small():
            remote(su * 2 + pc, np_send.at[k], npu_recv.at[k], partner, news).wait_recv()
            acc_new[...] += new_dot(su)

            @pl.when(k < 7)
            def _():
                remote(sd * 2 + pc, np_send.at[k], npd_recv.at[k], partner, news).wait_recv()
                acc_new[...] += new_dot(sd)

        if isinstance(t, int):
            if t % NCH == 0:
                small()
        else:
            pl.when(t % NCH == 0)(small)
        remote((su * 2 + pc) * NCH + cu, pt_send, pu_recv.at[t], partner).wait_recv()
        at = pl.ds(pl.multiple_of(cu * CH, CH), CH)
        acc[at, :] += kv_dot(su, cu)
        remote((sd * 2 + pc) * NCH + cd, pt_send, pd_recv.at[t], partner).wait_recv()
        at = pl.ds(pl.multiple_of(cd * CH, CH), CH)
        acc[at, :] += kv_dot(sd, cd)

    last = STEPS - HALF

    def step(t, carry):
        relay(t)
        pl.when(t >= 1)(lambda: compute(t - 1))
        return carry

    lax.fori_loop(0, last + 1, step, 0)

    def turned(x, cosine, sine):
        swapped = jnp.where(first, pltpu.roll(x, LANES - 32, 1), pltpu.roll(x, 32, 1))
        return x * cosine + swapped * sine

    told(2)

    def head_sums(v):
        lo = jnp.sum(jnp.where(low, v, 0.0), axis=1, keepdims=True)
        hi = jnp.sum(jnp.where(low, 0.0, v), axis=1, keepdims=True)
        return jnp.where(low, lo, hi)

    one = jnp.exp(ld)

    def query_of_new():
        new_angle = (groups * span) * inverse
        new_cos = jnp.cos(new_angle)
        new_sin = jnp.where(first, -jnp.sin(new_angle), jnp.sin(new_angle))
        new_k = (turned(acc_new[0:8, 0:128], new_cos, new_sin) * 0.125).astype(jnp.bfloat16)
        new_v = acc_new[0:8, 128:256].astype(jnp.bfloat16).astype(jnp.float32)
        new_q = turned(acc_new[0:8, 256:384], new_cos, new_sin).astype(jnp.bfloat16)
        new_q = new_q.astype(jnp.float32)
        return new_q, head_sums(new_q * new_k.astype(jnp.float32)) * new_v

    def part_of(p, part):
        at = pl.ds(part * CH, CH)
        rows = acc[pl.ds((part * 3 + p) * CH, CH), :]
        keys = turned(rows[:, 0:128], cos_t[at, :], sin_t[at, :]).astype(jnp.bfloat16)
        keys = (keys.astype(jnp.float32) * dec_t[at, :]).astype(jnp.bfloat16)
        return lax.dot_general(
            keys,
            rows[:, 128:256].astype(jnp.bfloat16),
            (((0,), (0,)), ((), ())),
            preferred_element_type=jnp.float32,
        )

    def hand_out(p, total):
        tile = jnp.where(low, total[0:HD, :], total[HD:, :]) * carried
        query = jnp.where(low, q_cols[0:HD, p : p + 1], q_cols[HD:, p : p + 1])
        partial = jnp.sum(tile * query, axis=0, keepdims=True) * one
        packed = [
            tile.reshape(groups, HD // groups, LANES),
            jnp.broadcast_to(partial[None], (groups, 1, LANES)),
            jnp.zeros((groups, 3, LANES), jnp.float32),
        ]
        out_buf[p] = jnp.concatenate(packed, axis=1).astype(jnp.bfloat16)
        for dy, dx in OTHERS:
            peer = ((y + dy) % 4) * 4 + (x + dx) % 4
            pltpu.make_async_remote_copy(
                src_ref=out_buf.at[p, peer],
                dst_ref=in_buf.at[p, sp],
                send_sem=x_send.at[p],
                recv_sem=x_recv.at[p],
                device_id=(peer, tp),
                device_id_type=MESH,
            ).start()
        in_buf[p, sp] = out_buf[p, sp]

    def arrived(p):
        view = in_buf.at[p, pl.ds(0, groups - 1)]
        pltpu.make_async_copy(view, view, x_recv.at[p]).wait()
        parts = [in_buf[p, d].astype(jnp.float32) for d in range(groups)]
        while len(parts) > 1:
            parts = [parts[i] + parts[i + 1] for i in range(0, len(parts), 2)]
        whole = parts[0]
        rows = whole[0:4, :].astype(jnp.bfloat16)
        state_ref[p, 0] = rows[:, 0:HD]
        state_ref[p, 1] = rows[:, HD:]
        raw = whole[4:5, :] + own_term[p : p + 1, :]
        centered = raw - head_sums(raw) * (1.0 / HD)
        scale = lax.rsqrt(head_sums(centered * centered) * (1.0 / HD) + 1e-05)
        read_ref[pl.ds(p, 1), :] = (centered * scale).astype(jnp.bfloat16)

    totals = [None] * 3
    for pos in range(HALF):
        if pos + 1 < HALF:
            relay(last + pos + 1)
        compute(last + pos)
        if pos == 0:
            new_q, own_term = query_of_new()
            q_cols = jnp.transpose(jnp.concatenate([new_q] * 16, axis=0))
        p, part = pos % 3, pos // 3
        both = part_of(p, part) + part_of(p, part + PARTS // 2)
        totals[p] = both if totals[p] is None else totals[p] + both
        if part == PARTS // 2 - 1:
            hand_out(p, totals[p])
    for p in range(3):
        arrived(p)

    def drain(view, sem):
        pltpu.make_async_copy(view, view, sem).wait()

    drain(blocks.at[pl.ds(0, STEPS)], up_send)
    drain(blocks.at[pl.ds(0, STEPS)], dn_send)
    drain(blocks.at[pl.ds(0, 2 * STEPS + NCH)], pt_send)
    for k in range(8):
        drain(news.at[0], nu_send.at[k])
    for k in range(7):
        drain(news.at[0], nd_send.at[k])
    for k in range(16):
        drain(news.at[0], np_send.at[k])
    for p in range(3):
        drain(in_buf.at[p, pl.ds(0, groups - 1)], x_send.at[p])


def body(tokens, new_token, query_weight, key_weight, value_weight, log_decay):
    groups = lax.axis_size("sp")
    n_tp = lax.axis_size("tp")
    depth = n_tp * LANES
    dma = pltpu.SemaphoreType.DMA
    anywhere = pl.BlockSpec(memory_space=pltpu.HBM)
    vmem = pl.BlockSpec(memory_space=pltpu.VMEM)
    return pl.pallas_call(
        functools.partial(kernel, groups),
        out_shape=(
            jax.ShapeDtypeStruct((3, 2, HD // groups, HD), jnp.bfloat16),
            jax.ShapeDtypeStruct((3, LANES), jnp.bfloat16),
        ),
        in_specs=[
            anywhere,
            vmem,
            anywhere,
            anywhere,
            anywhere,
            vmem,
        ],
        out_specs=(vmem, vmem),
        scratch_shapes=[
            pltpu.VMEM((n_tp * NCH, CH, LANES), jnp.bfloat16),
            pltpu.VMEM((n_tp, 8, LANES), jnp.bfloat16),
            pltpu.VMEM((depth, 3 * LANES), jnp.bfloat16),
            pltpu.VMEM((NCH * CH, 2 * LANES), jnp.float32),
            pltpu.VMEM((8, 3 * LANES), jnp.float32),
            pltpu.VMEM((PARTS * CH, LANES), jnp.float32),
            pltpu.VMEM((PARTS * CH, LANES), jnp.float32),
            pltpu.VMEM((PARTS * CH, LANES), jnp.float32),
            pltpu.VMEM((3, groups, 8, LANES), jnp.bfloat16),
            pltpu.VMEM((3, groups, 8, LANES), jnp.bfloat16),
            dma((NCH,)),
            dma((3,)),
            dma,
            dma,
            dma,
            dma((STEPS,)),
            dma((STEPS,)),
            dma((STEPS,)),
            dma((STEPS,)),
            dma((NCH,)),
            dma((8,)),
            dma((7,)),
            dma((16,)),
            dma((8,)),
            dma((7,)),
            dma((8,)),
            dma((7,)),
            dma,
            dma((3,)),
            dma((3,)),
            pltpu.SemaphoreType.REGULAR((3,)),
        ],
        compiler_params=pltpu.CompilerParams(
            collective_id=0, has_side_effects=True, vmem_limit_bytes=55112 * 1024
        ),
    )(tokens, new_token[:, 0, :], query_weight, key_weight, value_weight, log_decay[None])


def solution(mesh):
    return jax.shard_map(
        body,
        mesh=mesh,
        in_specs=(
            P(None, "sp", "tp"),
            P(None, None, "tp"),
            P(None, "tp"),
            P(None, "tp"),
            P(None, "tp"),
            P("tp"),
        ),
        out_specs=(P(None, "tp", "sp", None), P(None, "tp")),
        check_vma=False,
    )
```

```python
import functools

import jax
import jax.numpy as jnp
import numpy as np
from jax import lax
from jax.experimental import pallas as pl
from jax.experimental.pallas import tpu as pltpu
from jax.sharding import PartitionSpec as P

HD = 64
MESH = pl.DeviceIdType.MESH
NZ = 16
CH = 256
PARTS = 2
NCH = 3 * PARTS
HALF = NCH // 2
STEPS = 7 * NCH + HALF
LANES = 128
OTHERS = sorted(
    ((dy, dx) for dy in range(4) for dx in range(4) if dy or dx),
    key=lambda d: -sum(min(v, 4 - v) for v in d),
)


def kernel(
    groups,
    tok_ref,
    new_ref,
    wq_ref,
    wk_ref,
    wv_ref,
    ld_ref,
    state_ref,
    read_ref,
    blocks,
    news,
    weights,
    acc,
    acc_new,
    cos_t,
    sin_t,
    dec_t,
    out_buf,
    in_buf,
    tok_sem,
    w_sem,
    up_send,
    dn_send,
    pt_send,
    up_recv,
    dn_recv,
    pu_recv,
    pd_recv,
    own_recv,
    nu_send,
    nd_send,
    np_send,
    nu_recv,
    nd_recv,
    npu_recv,
    npd_recv,
    nown_recv,
    x_send,
    x_recv,
    ready,
):
    sp = lax.axis_index("sp")
    tp = lax.axis_index("tp")
    z = tp // 2
    y, x = sp // 4, sp % 4
    core = tp % 2
    up = ((z + 1) % NZ) * 2 + core
    dn = ((z + NZ - 1) % NZ) * 2 + core
    partner = z * 2 + (1 - core)
    span = PARTS * CH

    barrier = pltpu.get_barrier_semaphore()
    for peer in (up, dn, partner):
        pl.semaphore_signal(barrier, inc=1, device_id=(sp, peer), device_id_type=MESH)
    beside = [y * 4 + (x + d) % 4 for d in (1, 3)] + [((y + d) % 4) * 4 + x for d in (1, 3)]
    for peer in beside:
        pl.semaphore_signal(barrier, inc=1, device_id=(peer, tp), device_id_type=MESH)

    own_copies = []
    for ch in range(NCH):
        part, p = ch // 3, ch % 3
        c = pltpu.make_async_copy(
            tok_ref.at[p, pl.ds(part * CH, CH), :], blocks.at[tp * NCH + ch], tok_sem.at[ch]
        )
        c.start()
        own_copies.append(c)
    w_copies = []
    for i, ref in enumerate((wk_ref, wv_ref, wq_ref)):
        c = pltpu.make_async_copy(ref, weights.at[:, pl.ds(i * LANES, LANES)], w_sem.at[i])
        c.start()
        w_copies.append(c)

    own_new = jnp.concatenate(
        [new_ref[...].astype(jnp.float32), jnp.zeros((5, LANES), jnp.float32)], axis=0
    )
    news[tp] = own_new.astype(jnp.bfloat16)

    pl.semaphore_wait(barrier, 3 + 4)

    def tell(r):
        for peer in beside:
            pl.semaphore_signal(ready.at[r], inc=1, device_id=(peer, tp), device_id_type=MESH)

    def told(r):
        pl.semaphore_wait(ready.at[r], 4)

    tell(0)

    def remote(src, send, recv, peer, ref=None):
        ref = blocks if ref is None else ref
        return pltpu.make_async_remote_copy(
            src_ref=ref.at[src],
            dst_ref=ref.at[src],
            send_sem=send,
            recv_sem=recv,
            device_id=(sp, peer),
            device_id_type=MESH,
        )

    remote(tp, nu_send.at[0], nu_recv.at[0], up, news).start()
    remote(tp, nd_send.at[0], nd_recv.at[0], dn, news).start()
    remote(tp, np_send.at[15], nown_recv, partner, news).start()
    for pos in range(NCH):
        cu, cd = pos, (pos + HALF) % NCH
        if pos < HALF:
            own_copies[cu].wait()
            own_copies[cd].wait()
        remote(tp * NCH + cu, up_send, up_recv.at[pos], up).start()
        remote(tp * NCH + cd, dn_send, dn_recv.at[pos], dn).start()
    for ch in range(NCH):
        remote(tp * NCH + ch, pt_send, own_recv.at[ch], partner).start()

    def source(t, down):
        k, pos = t // NCH, t % NCH
        if down:
            sz = (z + 1 + k) % NZ
            ch = (pos + HALF) % NCH
        else:
            sz = (z + NZ - 1 - k) % NZ
            ch = pos
        return k, sz, ch

    lane = lax.broadcasted_iota(jnp.int32, (1, LANES), 1)
    inverse = jnp.zeros((1, LANES), jnp.float32)
    freq = (10000.0 ** (-np.arange(32, dtype=np.float64) / 32)).astype(np.float32)
    for i in range(32):
        inverse = jnp.where(lane % 32 == i, float(freq[i]), inverse)
    first = (lane % HD) < 32
    low = lane < HD
    ld = jnp.where(low, ld_ref[0:1, 0:1], ld_ref[0:1, 1:2])
    row = lax.broadcasted_iota(jnp.int32, (span, LANES), 0)
    angle = (row + sp * span).astype(jnp.float32) * inverse
    cos_t[...] = jnp.cos(angle) * 0.125
    sin_t[...] = jnp.where(first, -jnp.sin(angle), jnp.sin(angle)) * 0.125
    dec_t[...] = jnp.exp((span - 1 - row).astype(jnp.float32) * ld)
    carried = jnp.exp(ld * (span * (groups - 1 - sp)).astype(jnp.float32))

    told(0)
    tell(1)
    for c in w_copies:
        c.wait()

    def lhs(sz, ch):
        return jnp.concatenate(
            [blocks[(2 * sz) * NCH + ch], blocks[(2 * sz + 1) * NCH + ch]], axis=1
        )

    def rows_of(sz):
        return pl.ds(pl.multiple_of(sz * 256, 256), 256)

    def new_dot(sz):
        x = jnp.concatenate([news[2 * sz], news[2 * sz + 1]], axis=1)
        return jnp.dot(x, weights[rows_of(sz), :], preferred_element_type=jnp.float32)

    def kv_dot(sz, ch):
        return jnp.dot(
            lhs(sz, ch), weights[rows_of(sz), 0:256], preferred_element_type=jnp.float32
        )

    remote(partner, np_send.at[15], nown_recv, partner, news).wait_recv()
    acc_new[...] = new_dot(z)
    for ch in range(NCH):
        remote(partner * NCH + ch, pt_send, own_recv.at[ch], partner).wait_recv()
        acc[pl.ds(ch * CH, CH), :] = kv_dot(z, ch)

    told(1)
    tell(2)

    def relay(t):
        k, su, cu = source(t, False)
        _, sd, cd = source(t, True)
        bu = (su * 2 + core) * NCH + cu
        bd = (sd * 2 + core) * NCH + cd

        def small():
            nu = su * 2 + core
            nd = sd * 2 + core
            remote(nu, nu_send.at[k], nu_recv.at[k], up, news).wait_recv()

            @pl.when(k < 7)
            def _():
                remote(nu, nu_send.at[k + 1], nu_recv.at[k + 1], up, news).start()
                remote(nd, nd_send.at[k], nd_recv.at[k], dn, news).wait_recv()

                @pl.when(k < 6)
                def _():
                    remote(nd, nd_send.at[k + 1], nd_recv.at[k + 1], dn, news).start()

                remote(nd, np_send.at[k + 8], npd_recv.at[k], partner, news).start()

            remote(nu, np_send.at[k], npu_recv.at[k], partner, news).start()

        if isinstance(t, int):
            if t % NCH == 0:
                small()
        else:
            pl.when(t % NCH == 0)(small)

        def forward():
            remote(bu, up_send, up_recv.at[t + NCH], up).start()

        def forward_down():
            remote(bd, dn_send, dn_recv.at[t + NCH], dn).start()

        remote(bu, up_send, up_recv.at[t], up).wait_recv()
        if isinstance(t, int):
            if t + NCH < STEPS:
                forward()
        else:
            pl.when(t + NCH < STEPS)(forward)
        remote(bu, pt_send, pu_recv.at[t], partner).start()
        remote(bd, dn_send, dn_recv.at[t], dn).wait_recv()
        if isinstance(t, int):
            if t + NCH < STEPS:
                forward_down()
        else:
            pl.when(t + NCH < STEPS)(forward_down)
        remote(bd, pt_send, pd_recv.at[t], partner).start()

    def compute(t):
        k, su, cu = source(t, False)
        _, sd, cd = source(t, True)
        pc = 1 - core

        def small():
            remote(su * 2 + pc, np_send.at[k], npu_recv.at[k], partner, news).wait_recv()
            acc_new[...] += new_dot(su)

            @pl.when(k < 7)
            def _():
                remote(sd * 2 + pc, np_send.at[k], npd_recv.at[k], partner, news).wait_recv()
                acc_new[...] += new_dot(sd)

        if isinstance(t, int):
            if t % NCH == 0:
                small()
        else:
            pl.when(t % NCH == 0)(small)
        remote((su * 2 + pc) * NCH + cu, pt_send, pu_recv.at[t], partner).wait_recv()
        at = pl.ds(pl.multiple_of(cu * CH, CH), CH)
        acc[at, :] += kv_dot(su, cu)
        remote((sd * 2 + pc) * NCH + cd, pt_send, pd_recv.at[t], partner).wait_recv()
        at = pl.ds(pl.multiple_of(cd * CH, CH), CH)
        acc[at, :] += kv_dot(sd, cd)

    last = STEPS - HALF

    def step(t, carry):
        relay(t)
        pl.when(t >= 1)(lambda: compute(t - 1))
        return carry

    lax.fori_loop(0, last + 1, step, 0)

    def turned(x, cosine, sine):
        swapped = jnp.where(first, pltpu.roll(x, LANES - 32, 1), pltpu.roll(x, 32, 1))
        return x * cosine + swapped * sine

    told(2)

    def head_sums(v):
        lo = jnp.sum(jnp.where(low, v, 0.0), axis=1, keepdims=True)
        hi = jnp.sum(jnp.where(low, 0.0, v), axis=1, keepdims=True)
        return jnp.where(low, lo, hi)

    one = jnp.exp(ld)

    def query_of_new():
        new_angle = (groups * span) * inverse
        new_cos = jnp.cos(new_angle)
        new_sin = jnp.where(first, -jnp.sin(new_angle), jnp.sin(new_angle))
        new_k = (turned(acc_new[0:8, 0:128], new_cos, new_sin) * 0.125).astype(jnp.bfloat16)
        new_v = acc_new[0:8, 128:256].astype(jnp.bfloat16).astype(jnp.float32)
        new_q = turned(acc_new[0:8, 256:384], new_cos, new_sin).astype(jnp.bfloat16)
        new_q = new_q.astype(jnp.float32)
        return new_q, head_sums(new_q * new_k.astype(jnp.float32)) * new_v

    def part_of(p, part, added=None):
        at = pl.ds(part * CH, CH)
        rows = acc[pl.ds((part * 3 + p) * CH, CH), :]
        if added is not None:
            rows = rows + added
        keys = turned(rows[:, 0:128], cos_t[at, :], sin_t[at, :]).astype(jnp.bfloat16)
        keys = (keys.astype(jnp.float32) * dec_t[at, :]).astype(jnp.bfloat16)
        return lax.dot_general(
            keys,
            rows[:, 128:256].astype(jnp.bfloat16),
            (((0,), (0,)), ((), ())),
            preferred_element_type=jnp.float32,
        )

    def hand_out(p, total):
        tile = jnp.where(low, total[0:HD, :], total[HD:, :]) * carried
        query = jnp.where(low, q_cols[0:HD, p : p + 1], q_cols[HD:, p : p + 1])
        partial = jnp.sum(tile * query, axis=0, keepdims=True) * one
        packed = [
            tile.reshape(groups, HD // groups, LANES),
            jnp.broadcast_to(partial[None], (groups, 1, LANES)),
            jnp.zeros((groups, 3, LANES), jnp.float32),
        ]
        out_buf[p] = jnp.concatenate(packed, axis=1).astype(jnp.bfloat16)
        for dy, dx in OTHERS:
            peer = ((y + dy) % 4) * 4 + (x + dx) % 4
            pltpu.make_async_remote_copy(
                src_ref=out_buf.at[p, peer],
                dst_ref=in_buf.at[p, sp],
                send_sem=x_send.at[p],
                recv_sem=x_recv.at[p],
                device_id=(peer, tp),
                device_id_type=MESH,
            ).start()
        in_buf[p, sp] = out_buf[p, sp]

    def arrived(p):
        view = in_buf.at[p, pl.ds(0, groups - 1)]
        pltpu.make_async_copy(view, view, x_recv.at[p]).wait()
        parts = [in_buf[p, d].astype(jnp.float32) for d in range(groups)]
        while len(parts) > 1:
            parts = [parts[i] + parts[i + 1] for i in range(0, len(parts), 2)]
        whole = parts[0]
        rows = whole[0:4, :].astype(jnp.bfloat16)
        state_ref[p, 0] = rows[:, 0:HD]
        state_ref[p, 1] = rows[:, HD:]
        raw = whole[4:5, :] + own_term[p : p + 1, :]
        centered = raw - head_sums(raw) * (1.0 / HD)
        scale = lax.rsqrt(head_sums(centered * centered) * (1.0 / HD) + 1e-05)
        read_ref[pl.ds(p, 1), :] = (centered * scale).astype(jnp.bfloat16)

    totals = [None] * 3
    for pos in range(HALF):
        if pos + 1 < HALF:
            relay(last + pos + 1)
        if pos == HALF - 1:
            t = last + pos
            _, su, cu = source(t, False)
            _, sd, cd = source(t, True)
            other = 1 - core
            remote((su * 2 + other) * NCH + cu, pt_send, pu_recv.at[t], partner).wait_recv()
            total = totals[2] if totals[2] is not None else 0.0
            total = total + part_of(2, cu // 3, kv_dot(su, cu))
            remote((sd * 2 + other) * NCH + cd, pt_send, pd_recv.at[t], partner).wait_recv()
            hand_out(2, total + part_of(2, cd // 3, kv_dot(sd, cd)))
            continue
        compute(last + pos)
        if pos == 0:
            new_q, own_term = query_of_new()
            q_cols = jnp.transpose(jnp.concatenate([new_q] * 16, axis=0))
        p, part = pos % 3, pos // 3
        both = part_of(p, part) + part_of(p, part + PARTS // 2)
        totals[p] = both if totals[p] is None else totals[p] + both
        if part == PARTS // 2 - 1:
            hand_out(p, totals[p])
    for p in range(3):
        arrived(p)

    def drain(view, sem):
        pltpu.make_async_copy(view, view, sem).wait()

    drain(blocks.at[pl.ds(0, STEPS)], up_send)
    drain(blocks.at[pl.ds(0, STEPS)], dn_send)
    drain(blocks.at[pl.ds(0, 2 * STEPS + NCH)], pt_send)
    for k in range(8):
        drain(news.at[0], nu_send.at[k])
    for k in range(7):
        drain(news.at[0], nd_send.at[k])
    for k in range(16):
        drain(news.at[0], np_send.at[k])
    for p in range(3):
        drain(in_buf.at[p, pl.ds(0, groups - 1)], x_send.at[p])


def body(tokens, new_token, query_weight, key_weight, value_weight, log_decay):
    groups = lax.axis_size("sp")
    n_tp = lax.axis_size("tp")
    depth = n_tp * LANES
    dma = pltpu.SemaphoreType.DMA
    anywhere = pl.BlockSpec(memory_space=pltpu.HBM)
    vmem = pl.BlockSpec(memory_space=pltpu.VMEM)
    return pl.pallas_call(
        functools.partial(kernel, groups),
        out_shape=(
            jax.ShapeDtypeStruct((3, 2, HD // groups, HD), jnp.bfloat16),
            jax.ShapeDtypeStruct((3, LANES), jnp.bfloat16),
        ),
        in_specs=[
            anywhere,
            vmem,
            anywhere,
            anywhere,
            anywhere,
            vmem,
        ],
        out_specs=(vmem, vmem),
        scratch_shapes=[
            pltpu.VMEM((n_tp * NCH, CH, LANES), jnp.bfloat16),
            pltpu.VMEM((n_tp, 8, LANES), jnp.bfloat16),
            pltpu.VMEM((depth, 3 * LANES), jnp.bfloat16),
            pltpu.VMEM((NCH * CH, 2 * LANES), jnp.float32),
            pltpu.VMEM((8, 3 * LANES), jnp.float32),
            pltpu.VMEM((PARTS * CH, LANES), jnp.float32),
            pltpu.VMEM((PARTS * CH, LANES), jnp.float32),
            pltpu.VMEM((PARTS * CH, LANES), jnp.float32),
            pltpu.VMEM((3, groups, 8, LANES), jnp.bfloat16),
            pltpu.VMEM((3, groups, 8, LANES), jnp.bfloat16),
            dma((NCH,)),
            dma((3,)),
            dma,
            dma,
            dma,
            dma((STEPS,)),
            dma((STEPS,)),
            dma((STEPS,)),
            dma((STEPS,)),
            dma((NCH,)),
            dma((8,)),
            dma((7,)),
            dma((16,)),
            dma((8,)),
            dma((7,)),
            dma((8,)),
            dma((7,)),
            dma,
            dma((3,)),
            dma((3,)),
            pltpu.SemaphoreType.REGULAR((3,)),
        ],
        compiler_params=pltpu.CompilerParams(
            collective_id=0, has_side_effects=True, vmem_limit_bytes=55112 * 1024
        ),
    )(tokens, new_token[:, 0, :], query_weight, key_weight, value_weight, log_decay[None])


def solution(mesh):
    return jax.shard_map(
        body,
        mesh=mesh,
        in_specs=(
            P(None, "sp", "tp"),
            P(None, None, "tp"),
            P(None, "tp"),
            P(None, "tp"),
            P(None, "tp"),
            P("tp"),
        ),
        out_specs=(P(None, "tp", "sp", None), P(None, "tp")),
        check_vma=False,
    )
```
